256 devices in a mesh: sp: 64 (over z, y, core), tp: 4 (over x).
Axes of the slice: x: 4, y: 4, z: 8, core: 2. Of those that a mesh axis runs over, the one named last changes fastest.
Arguments:
- conv_input: bfloat16 [16384, 2048], P('sp', 'tp'), may hold values from -6 to 6
- gate_branch: bfloat16 [16384, 2048], P('sp', 'tp'), may hold values from -6 to 6
- conv_taps: float32 [4, 2048], P(None, 'tp'), may hold values from -3 to 3
- narrow_maps: bfloat16 [2, 8, 128, 128], P(None, 'tp'), may hold values from -0.5 to 0.5
- wide_maps: bfloat16 [2, 4, 256, 256], P(None, 'tp'), may hold values from -0.375 to 0.375
- decay_param: float32 [2048], P('tp'), may hold values from 4.5 to 20
- decay_shift: float32 [16384, 2048], P('sp', 'tp'), may hold values from -0.75 to 0
- mixer_out: bfloat16 [2048, 2048], P('tp'), may hold values from -0.125 to 0.125
- stream: bfloat16 [16384, 2048], P(('sp', 'tp')), may hold values from -6 to 6
- norm_gain: float32 [2048], replicated, may hold values from 0.1 to 1.9
- routes: int32 [16384, 4], P('sp'), may hold values from 0 to 63, all different within a row; in each aligned block of 64 rows (0 to 63, 64 to 127, ...) at most 8 rows name the same one
- route_weights: float32 [16384, 4], P('sp'), may hold values from 0.05 to 0.5
- expert_gate: bfloat16 [64, 2048, 2048], P('sp', None, 'tp'), may hold values from -1 to 1
- expert_up: bfloat16 [64, 2048, 2048], P('sp', None, 'tp'), may hold values from -1 to 1
- expert_down: bfloat16 [64, 2048, 2048], P('sp', 'tp'), may hold values from -0.015625 to 0.015625
Outputs:
- layer_out: bfloat16 [16384, 2048], P(('sp', 'tp'))
The draws below stay inside these ranges and needn't reach their ends.
Inputs may be any that keep to these rules, and one draw needn't show every extreme that they name: `routes`: each row names 4 different experts. In each aligned block of 64 rows no expert is named more than 8 times, and in every draw some expert is named exactly 8 times in some block.
All inputs are finite; a program needn't handle non-finite values.
Results may differ from the reference program's by a relative error of at most 0.015.
Values may be sent and summed in bfloat16 or wider, within the bound.
A program may use at most 128 MiB of HBM per device.

```python
import math
import jax
import jax.numpy as jnp
import numpy as np
from jax import lax

D = 2048
HN = 128
HW = 256
WIDE_HEADS = 4
NARROW_HEADS = 8
RECURRENT_WIDTH = 2048
CONV = 4
FF = 2048
FF_PIECE = 512
TOP = 4
EXPERTS = 64
TOK_DEV = 256
TOK_LOCAL = 64
SEQUENCE_TOKENS = 16384
CAP = 8
N_TP = 4


def head_of_channel():
    channel = jnp.arange(RECURRENT_WIDTH, dtype=jnp.int32)
    segment = channel // (2 * HN + HW)
    within = channel % (2 * HN + HW)
    narrow_head = 2 * segment + within // HN
    return jnp.where(within < 2 * HN, narrow_head, 2 * WIDE_HEADS + segment)


def draw_decay_param(key, part):
    random_key_series = jax.random.split(jax.random.fold_in(key, 21), 3)
    fast_odds = 8
    fast_head = jax.random.randint(random_key_series[0], (3 * WIDE_HEADS,), 0, 16) < fast_odds
    fast_rate = jnp.exp(jax.random.uniform(random_key_series[1], (RECURRENT_WIDTH,), jnp.float32, math.log(1.0 / 50.0), math.log(1.0 / 30.0)))
    slow_rate = jnp.exp(jax.random.uniform(random_key_series[2], (RECURRENT_WIDTH,), jnp.float32, math.log(0.05), math.log(0.4))) / SEQUENCE_TOKENS
    step_rate = jnp.where(fast_head[head_of_channel()], fast_rate, slow_rate)
    return (-jnp.log(jnp.expm1(0.25 * step_rate))).astype(jnp.float32)


def draw_decay_shift(key, part):
    random_key_series = jax.random.split(jax.random.fold_in(key, 31), 3)
    block_count = SEQUENCE_TOKENS // TOK_DEV
    block_rate = jnp.exp(jax.random.uniform(random_key_series[0], (block_count, 1, RECURRENT_WIDTH), jnp.float32, math.log(0.1), math.log(1.0))) / SEQUENCE_TOKENS
    stable_level = -jnp.broadcast_to(block_rate, (block_count, TOK_DEV, RECURRENT_WIDTH)).reshape(SEQUENCE_TOKENS, RECURRENT_WIDTH)
    spike_position = jax.random.randint(random_key_series[1], (2,), 0, SEQUENCE_TOKENS)
    spike_hit = jnp.any(jnp.arange(SEQUENCE_TOKENS)[:, None] == spike_position[None, :], axis=1).astype(jnp.float32)
    spike_magnitude = jax.random.uniform(random_key_series[2], (1, RECURRENT_WIDTH), jnp.float32, math.log(0.5), math.log(0.8))
    return (stable_level + spike_hit[:, None] * spike_magnitude).astype(jnp.float32)


def expert_matrix(key, salt_value):
    key_pair = jax.random.split(jax.random.fold_in(key, salt_value), 2)
    column_scale = jnp.exp(jax.random.uniform(key_pair[0], (EXPERTS, FF), jnp.float32, math.log(0.5), math.log(12.0)))

    def one_expert(inputs):
        expert_index, scale_row = inputs
        expert_key = jax.random.fold_in(key_pair[1], expert_index)
        entries = jax.random.normal(expert_key, (D, FF), jnp.float32)
        return jnp.clip(entries * scale_row[None, :] * D ** (-0.5), -1.0, 1.0).astype(jnp.bfloat16)
    return lax.map(one_expert, (jnp.arange(EXPERTS), column_scale))


def draw_expert_gate(key, part):
    return expert_matrix(key, 41)


def draw_expert_up(key, part):
    return expert_matrix(key, 42)


def shard_levels(key, dims, cuts, least, high):
    loudness, own = 1.0, jax.random.fold_in(key, 6)
    for dim, blocks in cuts:
        heights = jnp.exp(jax.random.uniform(jax.random.fold_in(own, dim), (blocks,), jnp.float32, least / len(cuts), high / len(cuts)))
        loudness = loudness * jnp.repeat(heights, dims[dim] // blocks).reshape([-1 if axis == dim else 1 for axis in range(len(dims))])
    return loudness


def assign_block(key, own, number, rows, amount, top, limit, lean):
    sequence = jax.random.permutation(key, amount)
    packed, common = load_shares(amount, rows * top, limit, lean, True), load_shares(amount, rows * top, limit, lean, False)
    places = jnp.arange(amount)

    def named(sizes, turn):
        used = int((sizes > 0).sum())
        fixed = max(1, used // 4)
        moved = fixed + (places - fixed + turn * (used - fixed)) % max(1, amount - fixed)
        return jnp.zeros((amount,), jnp.int32).at[sequence[jnp.where(places < fixed, places, moved)]].set(jnp.asarray(sizes, jnp.int32))

    sizes = jnp.where(number % 4 == 0, named(packed, number // 4), named(common, number - number // 4 - 1))
    mixed = jax.random.permutation(jax.random.fold_in(own, 3), amount)
    source_of, sink = mixed[0:amount // 2 * 2:2], mixed[1:amount // 2 * 2:2]
    margin = jnp.minimum(sizes[source_of] - 1, limit - sizes[sink]) // 2
    margin = jnp.where((source_of == sequence[0]) | (sink == sequence[0]) | (sizes[sink] == 0), 0, jnp.maximum(margin, 0))
    moved = jax.random.randint(jax.random.fold_in(own, 4), (amount // 2,), 0, 1 << 20) % (margin + 1)
    sizes = sizes.at[source_of].add(-moved).at[sink].add(moved)
    labels = jnp.searchsorted(jnp.cumsum(sizes), jnp.arange(rows * top), side="right").astype(jnp.int32)
    grid = labels.reshape(top, rows).T
    grid = grid[jax.random.permutation(jax.random.fold_in(own, 1), rows)]
    turn = jax.random.randint(jax.random.fold_in(own, 2), (rows, 1), 0, top)
    return jnp.take_along_axis(grid, (jnp.arange(top)[None, :] + turn) % top, axis=1)


def load_shares(amount, total, most, lean, full):
    weights = [(1 << 20) // math.isqrt(rank ** lean) + 1 for rank in range(1, amount + 1)]
    largest = most if full else min(most, max(-(-total // amount), total * weights[0] // sum(weights)))
    least = 1 if total - largest >= amount - 1 else 0
    holding, rest = [largest] + [least] * (amount - 1), total - largest - least * (amount - 1)
    while rest > 0:
        movable = [i for i in range(1, amount) if holding[i] < largest] or [i for i in range(1, amount) if holding[i] < most]
        whole, budget = sum([weights[i] for i in movable]), rest
        for i in movable:
            extra = min(most - holding[i], max(1, budget * weights[i] // whole), rest)
            holding[i] = holding[i] + extra
            rest = rest - extra
    return np.array(holding)


def bell_draw(stream_key, shape, spread, reach, cuts=(), kind=jnp.bfloat16):
    drawn = spread * jax.random.normal(stream_key, shape, jnp.float32)
    if cuts:
        drawn = drawn * shard_levels(stream_key, shape, cuts, -0.22, 0.18)
    return jnp.clip(drawn, -reach, reach).astype(kind)


def setup_inputs(seed: int = 0) -> dict:
    key_list = jax.random.split(jax.random.key(seed), 16)
    conv_input = bell_draw(key_list[0], (SEQUENCE_TOKENS, RECURRENT_WIDTH), 1.0, 6.0, ((0, 64), (1, 4)))
    gate_branch = bell_draw(key_list[1], (SEQUENCE_TOKENS, RECURRENT_WIDTH), 1.0, 6.0, ((0, 64), (1, 4)))
    conv_taps = bell_draw(key_list[2], (CONV, RECURRENT_WIDTH), 0.5, 3.0, ((1, 4),), jnp.float32)
    narrow_maps = bell_draw(key_list[3], (2, NARROW_HEADS, HN, HN), HN ** -0.5, 0.5, ((1, 4),))
    wide_maps = bell_draw(key_list[4], (2, WIDE_HEADS, HW, HW), HW ** -0.5, 0.375, ((1, 4),))
    decay_param = draw_decay_param(jax.random.fold_in(key_list[15], 71), 0)
    decay_shift = draw_decay_shift(jax.random.fold_in(key_list[15], 71), 0)
    mixer_out = bell_draw(key_list[7], (RECURRENT_WIDTH, D), RECURRENT_WIDTH ** -0.5, 0.125, ((0, 4),))
    stream = bell_draw(key_list[8], (SEQUENCE_TOKENS, D), 1.0, 6.0, ((0, 256),))
    norm_gain = jnp.clip(1.0 + 0.18 * jax.random.normal(key_list[9], (D,), jnp.float32), 0.1, 1.9)
    routes_keys = jax.random.split(jax.random.fold_in(key_list[10], 1), SEQUENCE_TOKENS // TOK_LOCAL)
    routes_turns = jax.random.permutation(jax.random.fold_in(key_list[10], 3), SEQUENCE_TOKENS // TOK_LOCAL)
    routes = jax.vmap(lambda own, number: assign_block(jax.random.fold_in(key_list[10], 2), own, number, TOK_LOCAL, EXPERTS, TOP, CAP, 2))(routes_keys, routes_turns).reshape((SEQUENCE_TOKENS, TOP))
    route_weights = jnp.clip(0.05 + 0.45 * jax.random.uniform(key_list[11], (SEQUENCE_TOKENS, TOP), jnp.float32) ** shard_levels(key_list[11], (SEQUENCE_TOKENS, TOP), ((0, 64),), -0.2, 0.2), 0.05, 0.5)
    expert_gate = draw_expert_gate(jax.random.fold_in(key_list[15], 71), 0)
    expert_up = draw_expert_up(jax.random.fold_in(key_list[15], 71), 0)
    expert_down = bell_draw(key_list[14], (EXPERTS, FF, D), (FF * 64) ** -0.5, 0.015625, ((0, 64), (1, 4)))
    return dict(conv_input=conv_input, gate_branch=gate_branch, conv_taps=conv_taps, narrow_maps=narrow_maps, wide_maps=wide_maps, decay_param=decay_param, decay_shift=decay_shift, mixer_out=mixer_out, stream=stream, norm_gain=norm_gain, routes=routes, route_weights=route_weights, expert_gate=expert_gate, expert_up=expert_up, expert_down=expert_down)


NORM_EPSILON = 1e-06
CLAMP_LIMIT = 7.0
GATE_SLOPE = 1.702
DECAY_SCALE = 8.0

def combine_steps(earlier, later):
    return (earlier[0] * later[0], later[0] * earlier[1] + later[1])

def head_maps(convolved, narrow_maps, wide_maps):
    seq_rows = convolved.shape[0]
    segments = convolved.reshape(seq_rows, WIDE_HEADS, 2 * HN + HW).astype(jnp.float32)
    narrow = segments[:, :, :2 * HN].reshape(seq_rows, 2 * WIDE_HEADS, HN)
    wide_part = segments[:, :, 2 * HN:]
    narrow_pre = jnp.einsum('rhi,mhio->mrho', narrow, narrow_maps.astype(jnp.float32))
    wide_pre = jnp.einsum('rhi,mhio->mrho', wide_part, wide_maps.astype(jnp.float32))
    narrow_pre = narrow_pre.reshape(2, seq_rows, WIDE_HEADS, 2 * HN)
    return jnp.concatenate([narrow_pre, wide_pre], axis=3).reshape(2, seq_rows, RECURRENT_WIDTH)

def clamp_units(gate_pre, up_pre):
    clamped = jnp.minimum(gate_pre, CLAMP_LIMIT)
    upper = jnp.clip(up_pre, -CLAMP_LIMIT, CLAMP_LIMIT)
    return (upper + 1.0) * clamped * jax.nn.sigmoid(GATE_SLOPE * clamped)

def reference(conv_input, gate_branch, conv_taps, narrow_maps, wide_maps, decay_param, decay_shift, mixer_out, stream, norm_gain, routes, route_weights, expert_gate, expert_up, expert_down):
    padded = jnp.pad(conv_input.astype(jnp.float32), ((CONV - 1, 0), (0, 0)))
    convolved = jnp.zeros((SEQUENCE_TOKENS, RECURRENT_WIDTH), jnp.float32)
    for offset in range(CONV):
        convolved = convolved + padded[offset:offset + SEQUENCE_TOKENS] * conv_taps[offset]
    convolved = convolved.astype(jnp.bfloat16)
    gate_pre = head_maps(convolved, narrow_maps, wide_maps)
    log_decay = -DECAY_SCALE * jax.nn.sigmoid(gate_pre[0]) * jax.nn.softplus(-decay_param) + decay_shift
    driving = jnp.sqrt(-jnp.expm1(2.0 * log_decay)) * jax.nn.sigmoid(gate_pre[1]) * convolved.astype(jnp.float32)
    _, recurrent = lax.associative_scan(combine_steps, (jnp.exp(log_decay), driving), axis=0)
    gated_rows = (recurrent * jax.nn.gelu(gate_branch.astype(jnp.float32))).astype(jnp.bfloat16)
    mixer_sum = jnp.dot(gated_rows, mixer_out, preferred_element_type=jnp.float32)
    hidden = (stream.astype(jnp.float32) + mixer_sum).astype(jnp.bfloat16)
    hidden_f = hidden.astype(jnp.float32)
    normed = (hidden_f * lax.rsqrt(lax.optimization_barrier(jnp.mean(hidden_f * hidden_f, axis=-1, keepdims=True)) + NORM_EPSILON) * norm_gain).astype(jnp.bfloat16)
    blocks = SEQUENCE_TOKENS // TOK_LOCAL
    flat_routes = routes.reshape(blocks, TOK_LOCAL * TOP)
    onehot = (flat_routes[:, :, None] == jnp.arange(EXPERTS, dtype=jnp.int32)[None, None, :]).astype(jnp.int32)
    slot_rank = lax.optimization_barrier(jnp.sum(jnp.cumsum(onehot, axis=1) * onehot, axis=2)) - 1
    block_index = jnp.arange(blocks, dtype=jnp.int32)[:, None]
    slot_index = flat_routes * (blocks * CAP) + block_index * CAP + slot_rank
    token_index = block_index * TOK_LOCAL + jnp.arange(TOK_LOCAL * TOP, dtype=jnp.int32)[None, :] // TOP
    slot_token = jnp.zeros((EXPERTS * blocks * CAP,), jnp.int32).at[slot_index.reshape(-1)].set(token_index.reshape(-1).astype(jnp.int32))
    slot_weight = jnp.zeros((EXPERTS * blocks * CAP,), route_weights.dtype).at[slot_index.reshape(-1)].set(route_weights.reshape(-1))
    slot_token = slot_token.reshape(EXPERTS, blocks * CAP)
    slot_weight = slot_weight.reshape(EXPERTS, blocks * CAP)

    def one_expert(combined, inputs):
        tokens_here, weights_here, gate_here, up_here, down_here = inputs
        picked = normed[tokens_here]
        gate_val = jnp.dot(picked, gate_here, preferred_element_type=jnp.float32)
        up_val = jnp.dot(picked, up_here, preferred_element_type=jnp.float32)
        activation = clamp_units(gate_val, up_val).astype(jnp.bfloat16)
        summed = jnp.zeros((picked.shape[0], D), jnp.float32)
        for piece_index in range(N_TP):
            first = piece_index * FF_PIECE
            partial_value = jnp.dot(activation[:, first:first + FF_PIECE], down_here[first:first + FF_PIECE], preferred_element_type=jnp.float32).astype(jnp.bfloat16)
            partial_value = lax.optimization_barrier(partial_value)
            summed = summed + partial_value.astype(jnp.float32)
        expert_out = lax.optimization_barrier(summed.astype(jnp.bfloat16)).astype(jnp.float32)
        combined = combined.at[tokens_here].add(weights_here[:, None] * expert_out)
        return (combined, None)
    combined, _ = lax.scan(one_expert, jnp.zeros((SEQUENCE_TOKENS, D), jnp.float32), (slot_token, slot_weight, expert_gate, expert_up, expert_down))
    return (hidden_f + combined).astype(jnp.bfloat16)
```

```python
import jax
import jax.numpy as jnp
from jax import lax
from jax.experimental import pallas as pl
from jax.experimental.pallas import tpu as pltpu
from jax.sharding import PartitionSpec as P

NORM_EPSILON = 1e-06
CLAMP_LIMIT = 7.0
GATE_SLOPE = 1.702
DECAY_SCALE = 8.0
PLANE = 8
MESH = pl.DeviceIdType.MESH
F32 = jnp.float32
BF16 = jnp.bfloat16


def one_minus_exp(x):
    series = 1.0 + x * (1.0 / 9.0)
    for k in range(8, 1, -1):
        series = 1.0 + x * (1.0 / k) * series
    return jnp.where(x > -0.5, -x * series, 1.0 - jnp.exp(x))


def softplus_neg(p):
    u = jnp.exp(-p)
    series = u * (1.0 - u * (1.0 / 2 - u * (1.0 / 3 - u * (1.0 / 4 - u * (1.0 / 5)))))
    return jnp.where(u < 0.02, series, jnp.log(1.0 + u))


def gelu(x):
    inner = 0.7978845608028654 * (x + 0.044715 * x * x * x)
    return 0.5 * x * (1.0 + jnp.tanh(inner))


def sigmoid(x):
    return jax.nn.sigmoid(x)


def mixer_kernel(
    sp_count,
    tp_count,
    conv_ref,
    gate_ref,
    taps_ref,
    narrow_ref,
    wide_ref,
    decay_ref,
    shift_ref,
    mixer_ref,
    stream_ref,
    gain_ref,
    hidden_ref,
    normed_ref,
    halo,
    padded,
    gates,
    cum,
    local,
    comm_a,
    comm_b,
    gated,
    part,
    relay,
    final,
    halo_sems,
    a_sems,
    b_sems,
    r_sems,
):
    s = lax.axis_index("sp")
    x = lax.axis_index("tp")
    z, p = s // PLANE, s % PLANE
    z_count = sp_count // PLANE
    rows, channels = conv_ref.shape
    own = rows // tp_count
    half = own // 2

    def at_sp(i):
        return {"sp": i, "tp": x}

    def at_tp(i):
        return {"sp": s, "tp": i}

    right, left = lax.rem(x + 1, tp_count), lax.rem(x + tp_count - 1, tp_count)
    opposite = lax.rem(x + 2, tp_count)
    after, before = lax.rem(s + 1, sp_count), lax.rem(s + sp_count - 1, sp_count)
    barrier = pltpu.get_barrier_semaphore()
    partners = [at_sp(after), at_sp(before), at_tp(right), at_tp(left)]
    plane = [at_sp(z * PLANE + lax.rem(p + r, PLANE)) for r in range(1, PLANE)]
    column = [at_sp(lax.rem(z + r, z_count) * PLANE + p) for r in range(1, z_count)]
    partners += plane + column
    for to in partners:
        pl.semaphore_signal(barrier, inc=1, device_id=to, device_id_type=MESH)
    pl.semaphore_wait(barrier, len(partners))

    def copy(src, dst, sems, i, to):
        return pltpu.make_async_remote_copy(
            src_ref=src,
            dst_ref=dst,
            send_sem=sems.at[0, i],
            recv_sem=sems.at[1, i],
            device_id=to,
            device_id_type=MESH,
        )

    halo_copy = copy(conv_ref.at[pl.ds(rows - 16, 16)], halo, halo_sems, 0, at_sp(after))
    halo_copy.start()
    padded[pl.ds(16, rows), :] = conv_ref[...].astype(F32)
    halo_copy.wait()
    earlier = halo[...].astype(F32)
    padded[pl.ds(0, 16), :] = jnp.where(s == 0, jnp.zeros_like(earlier), earlier)
    taps = taps_ref[...]
    convolved = padded[pl.ds(13, rows), :] * taps[0:1]
    for k in range(1, 4):
        convolved = convolved + padded[pl.ds(13 + k, rows), :] * taps[k : k + 1]
    convolved = convolved.astype(BF16)
    width = narrow_ref.shape[3]
    heads = narrow_ref.shape[1]
    for m in range(2):
        for h in range(heads):
            cut = slice(h * width, (h + 1) * width)
            gates[m, :, cut] = jnp.dot(
                convolved[:, cut], narrow_ref[m, h], preferred_element_type=F32
            )
        gates[m, :, heads * width :] = jnp.dot(
            convolved[:, heads * width :], wide_ref[m, 0], preferred_element_type=F32
        )
    rate = softplus_neg(decay_ref[...])
    row = lax.broadcasted_iota(jnp.int32, (rows, 128), 0)
    for j in range(channels // 128):
        cut = slice(j * 128, (j + 1) * 128)
        log_decay = -DECAY_SCALE * sigmoid(gates[0, :, cut]) * rate[:, cut] + shift_ref[:, cut]
        b = (
            jnp.sqrt(one_minus_exp(2.0 * log_decay))
            * sigmoid(gates[1, :, cut])
            * convolved[:, cut].astype(F32)
        )
        a = jnp.exp(log_decay)
        step = 1
        while step < rows:
            if step < 8:
                a_back = jnp.where(row >= step, pltpu.roll(a, step, 0), 1.0)
                b_back = jnp.where(row >= step, pltpu.roll(b, step, 0), 0.0)
            else:
                a_back = jnp.concatenate([jnp.ones((step, 128), F32), a[: rows - step]], axis=0)
                b_back = jnp.concatenate([jnp.zeros((step, 128), F32), b[: rows - step]], axis=0)
            b = a * b_back + b
            a = a * a_back
            step *= 2
        cum[:, cut] = a
        local[:, cut] = b
        comm_a[p, pl.ds(j, 1), :] = a[rows - 1 :]
        comm_a[p, pl.ds(4 + j, 1), :] = b[rows - 1 :]

    sends = [
        copy(comm_a.at[p], comm_a.at[p], a_sems, r, to) for r, to in enumerate(plane)
    ]
    for c in sends:
        c.start()
    for j in range(channels // 128):
        cut = slice(j * 128, (j + 1) * 128)
        gates[0, :, cut] = gelu(gate_ref[:, cut].astype(F32))
    for c in sends:
        c.wait()
    a_before, b_before = jnp.ones((4, 128), F32), jnp.zeros((4, 128), F32)
    a_all, b_all = a_before, b_before
    for q in range(PLANE):
        a, b = comm_a[q, 0:4, :], comm_a[q, 4:8, :]
        inside = q < p
        b_before = jnp.where(inside, a * b_before + b, b_before)
        a_before = jnp.where(inside, a * a_before, a_before)
        b_all = a * b_all + b
        a_all = a * a_all
    comm_b[z, 0:4, :] = a_all
    comm_b[z, 4:8, :] = b_all
    sends = [
        copy(comm_b.at[z], comm_b.at[z], b_sems, r, to) for r, to in enumerate(column)
    ]
    for c in sends:
        c.start()
    for c in sends:
        c.wait()
    state = jnp.zeros((4, 128), F32)
    for q in range(z_count):
        state = jnp.where(q < z, comm_b[q, 0:4, :] * state + comm_b[q, 4:8, :], state)
    state = a_before * state + b_before
    for j in range(channels // 128):
        cut = slice(j * 128, (j + 1) * 128)
        recurrent = local[:, cut] + cum[:, cut] * state[j : j + 1, :]
        gated[:, cut] = (recurrent * gates[0, :, cut]).astype(BF16)
    features = mixer_ref.shape[1]
    for j in range(features // 512):
        cut = slice(j * 512, (j + 1) * 512)
        part[:, cut] = jnp.dot(
            gated[...], mixer_ref[:, cut], preferred_element_type=F32
        ).astype(BF16)

    def rows_of(o, first, count):
        return pl.ds(pl.multiple_of(o * own + first, half), count)

    to_right, to_left = at_tp(right), at_tp(left)
    out = [
        copy(part.at[rows_of(opposite, 0, half)], relay.at[0], r_sems, 0, to_right),
        copy(part.at[rows_of(opposite, half, half)], relay.at[1], r_sems, 1, to_left),
        copy(
            part.at[rows_of(right, half, half)],
            final.at[0, pl.ds(half, half)],
            r_sems,
            2,
            to_right,
        ),
        copy(
            part.at[rows_of(left, 0, half)], final.at[1, pl.ds(0, half)], r_sems, 3, to_left
        ),
        copy(
            part.at[rows_of(right, 0, half)], final.at[0, pl.ds(0, half)], r_sems, 4, to_right
        ),
        copy(
            part.at[rows_of(left, half, half)],
            final.at[1, pl.ds(half, half)],
            r_sems,
            5,
            to_left,
        ),
    ]
    for c in out[:4]:
        c.start()
    for side, (o, first) in enumerate(((right, 0), (left, half))):
        out[side].wait_recv()
        where = rows_of(o, first, half)
        part[where, :] = (part[where, :].astype(F32) + relay[side].astype(F32)).astype(BF16)
        out[4 + side].start()
    base = stream_ref[...].astype(F32) + part[rows_of(x, 0, own), :].astype(F32)
    for c in out[2:]:
        c.wait_recv()
    hidden = (base + (final[0].astype(F32) + final[1].astype(F32))).astype(BF16)
    hidden_ref[...] = hidden
    hidden_f = hidden.astype(F32)
    mean = jnp.mean(hidden_f * hidden_f, axis=-1, keepdims=True)
    normed_ref[...] = (hidden_f * lax.rsqrt(mean + NORM_EPSILON) * gain_ref[...]).astype(BF16)
    for c in out:
        c.wait_send()


def mixer_stage(
    sp_count,
    tp_count,
    conv_input,
    gate_branch,
    conv_taps,
    narrow_maps,
    wide_maps,
    decay_param,
    decay_shift,
    mixer_out,
    stream,
    norm_gain,
):
    import functools

    rows, channels = conv_input.shape
    own, features = stream.shape
    vmem = pl.BlockSpec(memory_space=pltpu.VMEM)
    dma = pltpu.SemaphoreType.DMA
    return pl.pallas_call(
        functools.partial(mixer_kernel, sp_count, tp_count),
        out_shape=[jax.ShapeDtypeStruct((own, features), BF16)] * 2,
        in_specs=[vmem] * 10,
        out_specs=[vmem] * 2,
        scratch_shapes=[
            pltpu.VMEM((16, channels), BF16),
            pltpu.VMEM((rows + 16, channels), F32),
            pltpu.VMEM((2, rows, channels), F32),
            pltpu.VMEM((rows, channels), F32),
            pltpu.VMEM((rows, channels), F32),
            pltpu.VMEM((PLANE, 8, 128), F32),
            pltpu.VMEM((sp_count // PLANE, 8, 128), F32),
            pltpu.VMEM((rows, channels), BF16),
            pltpu.VMEM((rows, features), BF16),
            pltpu.VMEM((2, own // 2, features), BF16),
            pltpu.VMEM((2, own, features), BF16),
            dma((2, 1)),
            dma((2, PLANE - 1)),
            dma((2, sp_count // PLANE - 1)),
            dma((2, 6)),
        ],
        compiler_params=pltpu.CompilerParams(collective_id=0, has_side_effects=True),
    )(
        conv_input,
        gate_branch,
        conv_taps,
        narrow_maps,
        wide_maps,
        decay_param.reshape(1, -1),
        decay_shift,
        mixer_out,
        stream,
        norm_gain.reshape(1, -1),
    )


def cut_along(x, dim, length):
    lengths = x.shape
    blocks = x.reshape(*lengths[:dim], length, lengths[dim] // length, *lengths[dim + 1 :])
    return jnp.moveaxis(blocks, dim, 0)


def sum_at_owner(x, axis, dim):
    length = lax.axis_size(axis)
    blocks = lax.all_to_all(cut_along(x, dim, length), axis, 0, 0, tiled=True)
    return jnp.sum(blocks.astype(jnp.float32), axis=0)


def clamp_units(gate_pre, up_pre):
    clamped = jnp.minimum(gate_pre, CLAMP_LIMIT)
    upper = jnp.clip(up_pre, -CLAMP_LIMIT, CLAMP_LIMIT)
    return (upper + 1.0) * clamped * jax.nn.sigmoid(GATE_SLOPE * clamped)


def slot_ranks(flat_routes, expert_total):
    onehot = (
        flat_routes[:, :, None] == jnp.arange(expert_total, dtype=jnp.int32)[None, None, :]
    ).astype(jnp.int32)
    return jnp.sum(jnp.cumsum(onehot, axis=1) * onehot, axis=2) - 1


def take_rows(source_rows, slot_source):
    filled = slot_source >= 0
    picked = source_rows[jnp.maximum(slot_source, 0)]
    return jnp.where(filled[:, None], picked, jnp.zeros_like(picked))


def expert_work(arrived, expert_gate, expert_up, expert_down):
    local_experts = expert_gate.shape[0]
    buffer_shape = arrived.shape
    grouped = arrived.reshape(
        buffer_shape[0] // local_experts,
        local_experts,
        buffer_shape[1] * buffer_shape[2],
        buffer_shape[3],
    )
    gate_pre = jnp.einsum(
        "sxcd,xdf->sxcf", grouped, expert_gate, preferred_element_type=jnp.float32
    )
    up_pre = jnp.einsum("sxcd,xdf->sxcf", grouped, expert_up, preferred_element_type=jnp.float32)
    activation = clamp_units(gate_pre, up_pre).astype(jnp.bfloat16)
    partial_value = jnp.einsum(
        "sxcf,xfd->sxcd", activation, expert_down, preferred_element_type=jnp.float32
    )
    return partial_value.reshape(buffer_shape)


def shards(
    conv_input,
    gate_branch,
    conv_taps,
    narrow_maps,
    wide_maps,
    decay_param,
    decay_shift,
    mixer_out,
    stream,
    norm_gain,
    routes,
    route_weights,
    expert_gate,
    expert_up,
    expert_down,
):
    tp_count = lax.axis_size("tp")
    tok_local = stream.shape[0]
    hidden, normed = mixer_stage(
        lax.axis_size("sp"), tp_count, conv_input, gate_branch, conv_taps, narrow_maps,
        wide_maps, decay_param, decay_shift, mixer_out, stream, norm_gain,
    )
    hidden_f = hidden.astype(jnp.float32)
    model_width = normed.shape[1]
    top_count = routes.shape[1]
    expert_total = expert_gate.shape[0] * lax.axis_size("sp")
    capacity = max(2, 2 * tok_local * top_count // expert_total)
    own_index = lax.axis_index("tp")
    assignments = tok_local * top_count
    own_rows = lax.dynamic_slice_in_dim(routes, own_index * tok_local, tok_local, 0)
    own_routes = own_rows.reshape(assignments)
    own_ranks = slot_ranks(own_routes[None, :], expert_total)[0]
    source = jnp.arange(assignments, dtype=jnp.int32) // top_count
    slot_source = (
        jnp.full((expert_total * capacity,), -1, jnp.int32)
        .at[own_routes * capacity + own_ranks]
        .set(source)
    )
    outgoing = take_rows(normed, slot_source).reshape(expert_total, 1, capacity, model_width)
    partial_value = expert_work(
        lax.all_gather(
            lax.all_to_all(outgoing, "sp", split_axis=0, concat_axis=0, tiled=True),
            "tp",
            axis=1,
            tiled=True,
        ),
        expert_gate,
        expert_up,
        expert_down,
    )
    summed = sum_at_owner(partial_value.astype(jnp.bfloat16), "tp", 1).astype(jnp.bfloat16)
    returned = lax.all_to_all(summed, "sp", split_axis=0, concat_axis=0, tiled=True)
    own_slots = own_routes * capacity + own_ranks
    picked = returned.reshape(expert_total * capacity, model_width)[own_slots]
    own_weights = lax.dynamic_slice_in_dim(route_weights, own_index * tok_local, tok_local, 0)
    combined = jnp.sum(
        picked.reshape(tok_local, top_count, model_width).astype(jnp.float32)
        * own_weights[:, :, None],
        axis=1,
    )
    return (hidden_f + combined).astype(jnp.bfloat16)


def solution(mesh):
    placed = (
        P("sp", "tp"),
        P("sp", "tp"),
        P(None, "tp"),
        P(None, "tp", None, None),
        P(None, "tp", None, None),
        P("tp"),
        P("sp", "tp"),
        P("tp", None),
        P(("sp", "tp"), None),
        P(),
        P("sp", None),
        P("sp", None),
        P("sp", None, "tp"),
        P("sp", None, "tp"),
        P("sp", "tp", None),
    )
    return jax.shard_map(
        shards, mesh=mesh, in_specs=placed, out_specs=P(("sp", "tp"), None), check_vma=False
    )
```
